256 devices in a mesh: sp: 32 (over z, y), tp: 8 (over x, core).
Axes of the slice: x: 4, y: 4, z: 8, core: 2. Of those that a mesh axis runs over, the one named last changes fastest.
Arguments:
- target: bfloat16 [4096, 2048], P(('sp', 'tp')), may hold values from -0.119628906 to 0.119628906
- source: bfloat16 [16384, 2048], P(('sp', 'tp')), may hold values from -6 to 6
- target_gain: float32 [1, 2048], replicated, may hold values from 0.1 to 16
- source_gain: float32 [1, 2048], replicated, may hold values from 0.1 to 16
- w_query: bfloat16 [1, 2048, 4096], P(None, None, 'tp'), may hold values from -0.125 to 0.125
- w_key: bfloat16 [1, 2048, 512], P(None, None, 'tp'), may hold values from -0.125 to 0.125
- w_value: bfloat16 [1, 2048, 512], P(None, None, 'tp'), may hold values from -0.125 to 0.125
- w_out: bfloat16 [1, 4096, 2048], P(None, 'tp'), may hold values from -0.09375 to 0.09375
- final_gain: float32 [2048], replicated, may hold values from 0.1 to 1.9
Outputs:
- decoded: bfloat16 [4096, 2048], P(('sp', 'tp'))
The draws below stay inside these ranges and needn't reach their ends.
All inputs are finite; a program needn't handle non-finite values.
Results may differ from the reference program's by a relative error of at most 0.023.
The reference program's roundings to bfloat16 on the way (of `normed_source`, `key_rows`, `queries` and `attended`) count: a program that leaves them out, or rounds other values in their place, can miss the bound.
Values may be sent and summed in bfloat16 or wider, within the bound.
No kernel may reach another device: no remote copies, remote signals or barrier semaphores. Data moves between devices by JAX's collectives and lax.ppermute only.
A program may use at most 128 MiB of HBM per device.

```python
import jax
import jax.numpy as jnp
from jax import lax

D = 2048
HEADS = 8
HD = 512
LAYERS = 1
TARGET_LEN = 4096
SOURCE_LEN = 16384


def draw_gain_table(key):
    return 1.3 * (1.0 + 0.18 * jnp.clip(jax.random.normal(key, (LAYERS, D), jnp.float32), -5.0, 5.0))


def draw_target_gain(key, part):
    return draw_gain_table(jax.random.fold_in(key, 11))


def draw_source_gain(key, part):
    return draw_gain_table(jax.random.fold_in(key, 23))


def shard_levels(own_key, extent, cuts, smallest, high):
    loudness, own = 1.0, jax.random.fold_in(own_key, 6)
    for position, parts in cuts:
        steps = jnp.exp(jax.random.uniform(jax.random.fold_in(own, position), (parts,), jnp.float32, smallest / len(cuts), high / len(cuts)))
        loudness = loudness * jnp.repeat(steps, extent[position] // parts).reshape([-1 if axis == position else 1 for axis in range(len(extent))])
    return loudness


def bell_draw(own_key, dims, spread, bound, split=(), kind=jnp.bfloat16):
    drawn = spread * jax.random.normal(own_key, dims, jnp.float32)
    if split:
        drawn = drawn * shard_levels(own_key, dims, split, -0.22, 0.18)
    return jnp.clip(drawn, -bound, bound).astype(kind)


def setup_inputs(seed: int = 0) -> dict:
    key_list = jax.random.split(jax.random.key(seed), 10)
    target = bell_draw(key_list[0], (TARGET_LEN, D), 0.02, 0.119628906, ((0, 256),))
    source = bell_draw(key_list[1], (SOURCE_LEN, D), 1.0, 6.0, ((0, 256),))
    target_gain = draw_target_gain(jax.random.fold_in(key_list[9], 71), 0)
    source_gain = draw_source_gain(jax.random.fold_in(key_list[9], 71), 0)
    w_query = bell_draw(key_list[4], (LAYERS, D, HEADS * HD), D ** -0.5, 0.125, ((2, 8),))
    w_key = bell_draw(key_list[5], (LAYERS, D, HD), D ** -0.5, 0.125, ((2, 8),))
    w_value = bell_draw(key_list[6], (LAYERS, D, HD), D ** -0.5, 0.125, ((2, 8),))
    w_out = bell_draw(key_list[7], (LAYERS, HEADS * HD, D), (HEADS * HD) ** -0.5, 0.09375, ((1, 8),))
    final_gain = jnp.clip(1.0 + 0.18 * jax.random.normal(key_list[8], (D,), jnp.float32), 0.1, 1.9)
    return {"target": target, "source": source, "target_gain": target_gain, "source_gain": source_gain, "w_query": w_query, "w_key": w_key, "w_value": w_value, "w_out": w_out, "final_gain": final_gain}


EPSILON = 1e-06

def norm_rows(matrix, gain):
    values32 = matrix.astype(jnp.float32)
    scale = lax.rsqrt(lax.optimization_barrier(jnp.mean(values32 * values32, axis=-1, keepdims=True)) + EPSILON)
    return values32 * scale * gain.astype(jnp.float32)

def reference(target, source, target_gain, source_gain, w_query, w_key, w_value, w_out, final_gain):
    stream = target.astype(jnp.float32)
    target_rows = target.shape[0]
    for layer_index in range(LAYERS):
        normed_source = norm_rows(source, source_gain[layer_index]).astype(jnp.bfloat16)
        key_rows = jnp.dot(normed_source, w_key[layer_index], preferred_element_type=jnp.float32).astype(jnp.bfloat16)
        value_rows = jnp.dot(normed_source, w_value[layer_index], preferred_element_type=jnp.float32).astype(jnp.bfloat16)
        normed = norm_rows(stream, target_gain[layer_index]).astype(jnp.bfloat16)
        queries = jnp.dot(normed, w_query[layer_index], preferred_element_type=jnp.float32).astype(jnp.bfloat16)
        per_head = queries.reshape(target_rows, HEADS, HD).transpose(1, 0, 2)

        def attend(query_head):
            scores = jnp.dot(query_head, key_rows.T, preferred_element_type=jnp.float32) * HD ** (-0.5)
            row_top = lax.optimization_barrier(jnp.max(scores, axis=1, keepdims=True))
            weights = jnp.exp(scores - row_top)
            row_total = lax.optimization_barrier(jnp.sum(weights, axis=1, keepdims=True))
            numerator = jnp.dot(weights.astype(jnp.bfloat16), value_rows, preferred_element_type=jnp.float32)
            return (numerator / row_total).astype(jnp.bfloat16)
        heads_out = lax.map(attend, per_head)
        attended = heads_out.transpose(1, 0, 2).reshape(target_rows, HEADS * HD)
        stream = stream + jnp.dot(attended, w_out[layer_index], preferred_element_type=jnp.float32)
    return norm_rows(stream, final_gain).astype(jnp.bfloat16)
```

```python
import jax
import jax.numpy as jnp
from jax import lax
from jax.experimental import pallas as pl
from jax.experimental.pallas import tpu as pltpu
from jax.sharding import Mesh, PartitionSpec as P

HD = 512
EPSILON = 1e-06
BF = jnp.bfloat16
F32 = jnp.float32
NZ, NY, NX, NC = 8, 4, 4, 2
EXTRA = 16


def norm_rows(matrix, gain):
    values32 = matrix.astype(F32)
    scale = lax.rsqrt(jnp.mean(values32 * values32, axis=-1, keepdims=True) + EPSILON)
    return values32 * scale * gain


def moved(array, axis, shift):
    n = lax.axis_size(axis)
    return lax.ppermute(array, axis, [(i, (i + shift) % n) for i in range(n)])


def from_ring4(array, axis):
    far = moved(array, axis, 2)
    one = moved(array, axis, 1)
    back = moved(array, axis, -1)
    return [array, one, far, back]


def attend_kernel(*refs):
    q_refs = refs[:NZ]
    near, other = refs[NZ : NZ + 2]
    outs = refs[NZ + 2 : 2 * NZ + 2]
    keys, values_t, sems = refs[2 * NZ + 2 :]
    copies = []
    for part, blocks in enumerate((near, other)):
        for y in range(NY):
            row = part * 1024 + y * 256
            for x in range(NX):
                col = x * 128
                copies.append(pltpu.make_async_copy(
                    blocks.at[y, x, pl.ds(0, 256), :],
                    keys.at[pl.ds(row, 256), pl.ds(col, 128)], sems.at[len(copies)]))
                for half in range(2):
                    copies.append(pltpu.make_async_copy(
                        blocks.at[y, x, pl.ds(256 + half * 128, 128), :],
                        values_t.at[pl.ds(col, 128), pl.ds(row + half * 128, 128)],
                        sems.at[len(copies)]))
    for c in copies:
        c.start()
    for c in copies:
        c.wait()
    for pair in range(NZ // 2):
        q = jnp.concatenate([q_refs[2 * pair][...], q_refs[2 * pair + 1][...]], axis=0)
        scores = lax.dot_general(
            keys[...], q, (((1,), (1,)), ((), ())), preferred_element_type=F32
        ) * HD ** (-0.5)
        top = jnp.max(scores, axis=0, keepdims=True)
        weights = jnp.exp(scores - top)
        total = jnp.sum(weights, axis=0, keepdims=True)
        part = lax.dot_general(
            values_t[...], weights.astype(BF), (((1,), (0,)), ((), ())),
            preferred_element_type=F32) / total
        for side in range(2):
            out = outs[2 * pair + side]
            cols = slice(side * 128, side * 128 + 128)
            out[pl.ds(0, HD), :] = part[:, cols].astype(BF)
            pieces = []
            for stat in (top[:, cols], total[:, cols]):
                for _ in range(3):
                    piece = stat.astype(BF).astype(F32)
                    pieces.append(piece)
                    stat = stat - piece
            pieces.append(jnp.zeros((EXTRA - 6, 128), F32))
            out[pl.ds(HD, EXTRA), :] = jnp.concatenate(pieces, axis=0).astype(BF)


def attend(queries, near, other):
    vmem = pl.BlockSpec(memory_space=pltpu.VMEM)
    hbm = pl.BlockSpec(memory_space=pl.ANY)
    return pl.pallas_call(
        attend_kernel,
        out_shape=[jax.ShapeDtypeStruct((HD + EXTRA, 128), BF)] * NZ,
        in_specs=[vmem] * NZ + [hbm] * 2,
        out_specs=[vmem] * NZ,
        scratch_shapes=[
            pltpu.VMEM((2048, HD), BF),
            pltpu.VMEM((HD, 2048), BF),
            pltpu.SemaphoreType.DMA((96,)),
        ],
        cost_estimate=pl.CostEstimate(
            flops=4 * 1024 * 2048 * HD, bytes_accessed=8 << 20, transcendentals=1024 * 2048),
    )(*queries, near, other)


def on_device(target, source, target_gain, source_gain, w_query, w_key, w_value, w_out, final_gain):
    x = lax.axis_index("x")
    c = lax.axis_index("c")
    first = c == 0

    rows = norm_rows(source, source_gain[0]).astype(BF)
    row_blocks = from_ring4(rows, "x")

    stream = target.astype(F32)
    normed = norm_rows(stream, target_gain[0]).astype(BF)
    normed_other = moved(normed, "c", 1)
    chip_normed = jnp.concatenate(
        [jnp.where(first, normed, normed_other), jnp.where(first, normed_other, normed)], axis=0)
    target_blocks = from_ring4(chip_normed, "x")

    own_w = jnp.concatenate([w_key[0], w_value[0]], axis=1)
    other_w = moved(own_w, "c", 1)
    low = jnp.where(first, own_w, other_w)
    high = jnp.where(first, other_w, own_w)
    key_w = jnp.concatenate([low[:, :64], high[:, :64]], axis=1)
    value_w = jnp.concatenate([low[:, 64:], high[:, 64:]], axis=1)

    turn = (x - jnp.arange(NX)) % NX
    q_rot = jnp.dot(
        jnp.concatenate(target_blocks, axis=0), w_query[0], preferred_element_type=F32
    ).astype(BF)
    query = jnp.take(q_rot.reshape(NX, 32, HD), turn, axis=0).reshape(128, HD)
    queries = [query] + [moved(query, "z", k) for k in range(1, NZ)]

    gathered = jnp.take(jnp.stack(row_blocks), turn, axis=0).reshape(256, -1)
    keys = jnp.dot(gathered, key_w, preferred_element_type=F32).astype(BF)
    values_t = lax.dot_general(
        value_w, gathered, (((0,), (1,)), ((), ())), preferred_element_type=F32
    ).astype(BF)
    piece = jnp.concatenate([keys, values_t[:, :128], values_t[:, 128:]], axis=0)
    near = lax.all_to_all(
        jnp.broadcast_to(piece[None], (NY * NX, *piece.shape)), ("y", "x"), 0, 0, tiled=True
    ).reshape(NY, NX, *piece.shape)
    other = moved(near, "c", 1)

    parts = attend(queries, near, other)
    arrived = jnp.stack([parts[0]] + [moved(parts[k], "z", -k) for k in range(1, NZ)])
    stats = arrived[:, HD : HD + 6].astype(F32)
    tops = stats[:, 0] + stats[:, 1] + stats[:, 2]
    totals = stats[:, 3] + stats[:, 4] + stats[:, 5]
    shares = totals * jnp.exp(tops - jnp.max(tops, axis=0))
    shares = shares / jnp.sum(shares, axis=0)
    attended_t = jnp.sum(arrived[:, :HD].astype(F32) * shares[:, None, :], axis=0).astype(BF)

    projected = lax.dot_general(
        attended_t, w_out[0], (((0,), (0,)), ((), ())), preferred_element_type=F32)
    projected = projected.reshape(NX, NC, 16, -1)
    kept = jnp.where(first, projected[:, 0], projected[:, 1])
    sent = jnp.where(first, projected[:, 1], projected[:, 0]).astype(BF)
    chip_sum = kept + moved(sent, "c", 1).astype(F32)
    own_term = lax.dynamic_index_in_dim(chip_sum, x, 0, keepdims=False)
    rounded = chip_sum.astype(BF)
    total = stream + own_term
    for k in (2, 1, 3):
        block = lax.dynamic_index_in_dim(rounded, (x + k) % NX, 0, keepdims=False)
        total = total + moved(block, "x", k).astype(F32)
    return norm_rows(total, final_gain).astype(BF)


def solution(mesh):
    grid = Mesh(mesh.devices.reshape(NZ, NY, NX, NC), ("z", "y", "x", "c"))
    every = P(("z", "y", "x", "c"), None)
    in_specs = (
        every, every, P(), P(),
        P(None, None, ("x", "c")), P(None, None, ("x", "c")), P(None, None, ("x", "c")),
        P(None, ("x", "c"), None), P(),
    )
    return jax.shard_map(
        on_device, mesh=grid, in_specs=in_specs, out_specs=every, check_vma=False)
```

```python
import functools

import jax
import jax.numpy as jnp
from jax import lax
from jax.experimental import pallas as pl
from jax.experimental.pallas import tpu as pltpu
from jax.sharding import Mesh, PartitionSpec as P

HD = 512
EPSILON = 1e-06
BF = jnp.bfloat16
F32 = jnp.float32
NZ, NY, NX, NC = 8, 4, 4, 2
EXTRA = 16
VMEM = pl.BlockSpec(memory_space=pltpu.VMEM)
ANY = pl.BlockSpec(memory_space=pl.ANY)


def room(mib):
    return pltpu.CompilerParams(vmem_limit_bytes=mib << 20)


def norm_rows(matrix, gain):
    values32 = matrix.astype(F32)
    scale = lax.rsqrt(jnp.mean(values32 * values32, axis=-1, keepdims=True) + EPSILON)
    return values32 * scale * gain


def moved(array, axis, shift):
    n = lax.axis_size(axis)
    return lax.ppermute(array, axis, [(i, (i + shift) % n) for i in range(n)])


def ring4(array, axis):
    far = moved(array, axis, 2)
    one = moved(array, axis, 1)
    back = moved(array, axis, -1)
    return [array, one, far, back]


def norm_kernel(source, target, source_gain, target_gain, source_out, target_out):
    source_out[...] = norm_rows(source[...], source_gain[...]).astype(BF)
    target_out[...] = norm_rows(target[...], target_gain[...]).astype(BF)


def normed_inputs(source, target, source_gain, target_gain):
    return pl.pallas_call(
        norm_kernel,
        out_shape=[jax.ShapeDtypeStruct(source.shape, BF), jax.ShapeDtypeStruct(target.shape, BF)],
        in_specs=[VMEM] * 4,
        out_specs=[VMEM] * 2,
        compiler_params=room(8),
    )(source, target, source_gain, target_gain)


def key_value_kernel(*refs):
    blocks = refs[:NX]
    own_w, other_w, kept_out, sent_out, rows, sems = refs[NX:]
    x = lax.axis_index("x")
    first = lax.axis_index("c") == 0
    copies = []
    for k in range(NX):
        place = pl.multiple_of(lax.rem(x - k + NX, NX) * 64, 64)
        copies.append(pltpu.make_async_copy(blocks[k], rows.at[pl.ds(place, 64), :], sems.at[k]))
    for copy in copies:
        copy.start()
    for copy in copies:
        copy.wait()

    def projected(weight):
        return lax.dot_general(
            weight[...], rows[...], (((1,), (1,)), ((), ())), preferred_element_type=F32)

    own, other = projected(own_w), projected(other_w)
    low = jnp.where(first, own, other)
    high = jnp.where(first, other, own)
    keys = jnp.concatenate([low[:64], high[:64]], axis=0).T
    turned = jnp.concatenate([low[64:], high[64:]], axis=0)
    values = jnp.concatenate([turned[:, :128], turned[:, 128:]], axis=0)
    kept_out[...] = jnp.where(first, keys, values).astype(BF)
    sent_out[...] = jnp.where(first, values, keys).astype(BF)


def key_value(blocks, own_w, other_w):
    return pl.pallas_call(
        key_value_kernel,
        out_shape=[jax.ShapeDtypeStruct((256, 128), BF)] * 2,
        in_specs=[ANY] * NX + [VMEM] * 2,
        out_specs=[VMEM] * 2,
        scratch_shapes=[pltpu.VMEM((256, 2048), BF), pltpu.SemaphoreType.DMA((NX,))],
        compiler_params=room(12),
        cost_estimate=pl.CostEstimate(
            flops=2 * 256 * 2048 * 256, bytes_accessed=3 << 20, transcendentals=0),
    )(*blocks, own_w, other_w)


def query_kernel(*refs):
    weight, out, full = refs[NX:]
    x = lax.axis_index("x")
    rows = jnp.concatenate([ref[...] for ref in refs[:NX]], axis=0)
    full[...] = jnp.dot(rows, weight[...], preferred_element_type=F32)
    for k in range(NX):
        place = pl.multiple_of(lax.rem(x - k + NX, NX) * 128, 128)
        block = full[:, pl.ds(place, 128)].astype(BF)
        for copy in range(NZ):
            out[copy, :, pl.ds(k * 128, 128)] = block


def query_rows(blocks, weight):
    return pl.pallas_call(
        query_kernel,
        out_shape=jax.ShapeDtypeStruct((NZ, 128, HD), BF),
        in_specs=[VMEM] * (NX + 1),
        out_specs=VMEM,
        scratch_shapes=[pltpu.VMEM((128, HD), F32)],
        compiler_params=room(12),
        cost_estimate=pl.CostEstimate(
            flops=2 * 128 * 2048 * HD, bytes_accessed=3 << 20, transcendentals=0),
    )(*blocks, weight)


def soft_part(q, keys, values, outs):
    scores = []
    for m in range(NY):
        block = jnp.concatenate([keys[m, k] for k in range(NX)], axis=1)
        scores.append(lax.dot_general(
            block, q, (((1,), (1,)), ((), ())), preferred_element_type=F32) * HD ** (-0.5))
    top = functools.reduce(
        jnp.maximum, [jnp.max(score, axis=0, keepdims=True) for score in scores])
    total, numerator = 0.0, 0.0
    for m in range(NY):
        weights = jnp.exp(scores[m] - top)
        total = total + jnp.sum(weights, axis=0, keepdims=True)
        block = jnp.concatenate([
            jnp.concatenate(
                [values[k, m, pl.ds(row, 128), :] for row in (256, 384, 0, 128)], axis=1)
            for k in range(NX)], axis=0)
        numerator = numerator + jnp.dot(
            block, weights.astype(BF), preferred_element_type=F32)
    part = numerator / total
    for side, out in enumerate(outs):
        cols = slice(side * 128, side * 128 + 128)
        out[pl.ds(0, HD), :] = part[:, cols].astype(BF)
        pieces = []
        for stat in (top[:, cols], total[:, cols]):
            for _ in range(3):
                piece = stat.astype(BF).astype(F32)
                pieces.append(piece)
                stat = stat - piece
        pieces.append(jnp.zeros((EXTRA - 6, 128), F32))
        out[pl.ds(HD, EXTRA), :] = jnp.concatenate(pieces, axis=0).astype(BF)


def attend_kernel(*refs):
    n = (len(refs) - 11) // 2
    near, other = refs[n : n + NX], refs[n + NX : n + 2 * NX]
    outs = refs[n + 8 : 2 * n + 8]
    keys, values, sems = refs[2 * n + 8 :]
    core = lax.axis_index("c")

    def copies(key_blocks, value_blocks):
        return [
            pltpu.make_async_copy(block, place.at[i], sems.at[side * 4 + i])
            for side, (blocks, place) in enumerate(((key_blocks, keys), (value_blocks, values)))
            for i, block in enumerate(blocks)]

    @pl.when(core == 0)
    def _():
        for copy in copies(near, other):
            copy.start()

    @pl.when(core == 1)
    def _():
        for copy in copies(other, near):
            copy.start()

    for copy in copies(near, other):
        copy.wait()
    for i in range(0, n, 2):
        q = jnp.concatenate([ref[...] for ref in refs[i : i + 2]], axis=0)
        soft_part(q, keys, values, outs[i : i + 2])


def attend(queries, near, other):
    n = len(queries)
    return pl.pallas_call(
        attend_kernel,
        out_shape=[jax.ShapeDtypeStruct((HD + EXTRA, 128), BF)] * n,
        in_specs=[VMEM] * n + [ANY] * 8,
        out_specs=[VMEM] * n,
        scratch_shapes=[pltpu.VMEM((4, 4, 512, 128), BF)] * 2 + [pltpu.SemaphoreType.DMA((8,))],
        compiler_params=room(28),
        cost_estimate=pl.CostEstimate(
            flops=4 * 128 * n * 2048 * HD, bytes_accessed=4 << 20,
            transcendentals=n * 128 * 2048),
    )(*queries, *near, *other)


def combine_kernel(*refs):
    arrived = refs[:NZ]
    weight, kept, sent, attended = refs[NZ:]
    x = lax.axis_index("x")
    tops, totals = [], []
    for part in arrived:
        stats = part[pl.ds(HD, EXTRA), :].astype(F32)
        tops.append(stats[0:1] + stats[1:2] + stats[2:3])
        totals.append(stats[3:4] + stats[4:5] + stats[5:6])
    top = functools.reduce(jnp.maximum, tops)
    shares = [total * jnp.exp(t - top) for t, total in zip(tops, totals)]
    whole = sum(shares)
    shares = [share / whole for share in shares]
    for k in range(NX):
        block = sum(
            part[pl.ds(k * 128, 128), :].astype(F32) * share
            for part, share in zip(arrived, shares))
        place = pl.multiple_of(lax.rem(x - k + NX, NX) * 128, 128)
        attended[:, pl.ds(place, 128)] = block.T.astype(BF)
    projected = jnp.dot(attended[...], weight[...], preferred_element_type=F32)
    for k in range(NX):
        kept[pl.ds(k * 16, 16), :] = projected[k * 32 : k * 32 + 16]
        sent[pl.ds(k * 16, 16), :] = projected[k * 32 + 16 : k * 32 + 32].astype(BF)


def combine(arrived, weight):
    return pl.pallas_call(
        combine_kernel,
        out_shape=[jax.ShapeDtypeStruct((64, 2048), F32), jax.ShapeDtypeStruct((64, 2048), BF)],
        in_specs=[VMEM] * (NZ + 1),
        out_specs=[VMEM] * 2,
        scratch_shapes=[pltpu.VMEM((128, HD), BF)],
        compiler_params=room(16),
        cost_estimate=pl.CostEstimate(
            flops=2 * 128 * 2048 * HD, bytes_accessed=4 << 20, transcendentals=1024),
    )(*arrived, weight)


def pair_kernel(kept, met, own, *outs):
    own[...] = kept[pl.ds(0, 16), :] + met[pl.ds(0, 16), :].astype(F32)
    for k, out in enumerate(outs, 1):
        rows = pl.ds(k * 16, 16)
        out[...] = (kept[rows, :] + met[rows, :].astype(F32)).astype(BF)


def pair_sum(kept, met):
    return pl.pallas_call(
        pair_kernel,
        out_shape=[jax.ShapeDtypeStruct((16, 2048), F32)]
        + [jax.ShapeDtypeStruct((16, 2048), BF)] * 3,
        in_specs=[VMEM] * 2,
        out_specs=[VMEM] * 4,
        compiler_params=room(8),
    )(kept, met)


def last_kernel(target, own, one, two, three, gain, out):
    stream = target[...].astype(F32) + (
        own[...] + one[...].astype(F32) + two[...].astype(F32) + three[...].astype(F32))
    out[...] = norm_rows(stream, gain[...]).astype(BF)


def last_norm(*arrays):
    return pl.pallas_call(
        last_kernel,
        out_shape=jax.ShapeDtypeStruct((16, 2048), BF),
        in_specs=[VMEM] * 6,
        out_specs=VMEM,
        compiler_params=room(8),
    )(*arrays)


def by_role(array, shift, axes):
    pairs = []
    for y in range(NY):
        for x in range(NX):
            for core, axis in enumerate(axes):
                to_y = (y + shift) % NY if axis == "y" else y
                to_x = (x + shift) % NX if axis == "x" else x
                pairs.append((((y * NX) + x) * NC + core, ((to_y * NX) + to_x) * NC + core))
    return lax.ppermute(array, ("y", "x", "c"), pairs)


def role_ring4(array, axes):
    far = by_role(array, 2, axes)
    one = by_role(array, 1, axes)
    back = by_role(array, -1, axes)
    return [array, one, far, back]


def on_device(target, source, target_gain, source_gain, w_query, w_key, w_value, w_out, final_gain):
    rows, normed = normed_inputs(source, target, source_gain, target_gain)
    other_normed = moved(normed, "c", 1)
    rows, other_normed = lax.optimization_barrier((rows, other_normed))
    chip_normed = jnp.concatenate([normed, other_normed], axis=0)
    row_blocks = ring4(rows, "x")
    target_blocks = ring4(chip_normed, "x")
    copies = query_rows(target_blocks, w_query[0])
    queries = lax.all_to_all(copies, "z", 0, 0, tiled=True)

    own_w = jnp.concatenate([w_key[0].T, w_value[0].T], axis=0)
    other_w = moved(own_w, "c", 1)

    piece, sent = key_value(row_blocks, own_w, other_w)
    piece = jnp.concatenate([piece, moved(sent, "c", 1)], axis=0)
    line = jnp.stack(role_ring4(piece, ("x", "y")))
    near = role_ring4(line, ("y", "x"))
    other = [moved(block, "c", 1) for block in near]

    z = lax.axis_index("z")
    picked = [
        lax.dynamic_slice(queries, (lax.rem(z - k + NZ, NZ), 0, 0), (1, 128, HD)).reshape(128, HD)
        for k in range(NZ)]
    parts = dict(zip((4, 3), attend([picked[4], picked[3]], near, other)))
    arrived = []
    for k in (4, 3):
        arrived.append(moved(parts[k], "z", -k))
    rest = (5, 2, 6, 1, 7, 0)
    parts.update(zip(rest, attend([picked[k] for k in rest], near, other)))
    for k in rest[:-1]:
        arrived.append(moved(parts[k], "z", -k))
    arrived.append(parts[0])
    kept, sent = combine(arrived, w_out[0])
    met = moved(sent, "c", 1)
    own, one, two, three = pair_sum(kept, met)
    two = moved(two, "x", -2)
    one = moved(one, "x", -1)
    three = moved(three, "x", -3)
    return last_norm(target, own, one, two, three, final_gain.reshape(1, -1))


def solution(mesh):
    grid = Mesh(mesh.devices.reshape(NZ, NY, NX, NC), ("z", "y", "x", "c"))
    every = P(("z", "y", "x", "c"), None)
    in_specs = (
        every, every, P(), P(),
        P(None, None, ("x", "c")), P(None, None, ("x", "c")), P(None, None, ("x", "c")),
        P(None, ("x", "c"), None), P(),
    )
    return jax.shard_map(
        on_device, mesh=grid, in_specs=in_specs, out_specs=every, check_vma=False)
```

```python
import functools

import jax
import jax.numpy as jnp
from jax import lax
from jax.experimental import pallas as pl
from jax.experimental.pallas import tpu as pltpu
from jax.sharding import Mesh, PartitionSpec as P

HD = 512
EPSILON = 1e-06
BF = jnp.bfloat16
F32 = jnp.float32
NZ, NY, NX, NC = 8, 4, 4, 2
EXTRA = 16
VMEM = pl.BlockSpec(memory_space=pltpu.VMEM)
ANY = pl.BlockSpec(memory_space=pl.ANY)


def room(mib):
    return pltpu.CompilerParams(vmem_limit_bytes=mib << 20)


def norm_rows(matrix, gain):
    values32 = matrix.astype(F32)
    scale = lax.rsqrt(jnp.mean(values32 * values32, axis=-1, keepdims=True) + EPSILON)
    return values32 * scale * gain


def moved(array, axis, shift):
    n = lax.axis_size(axis)
    return lax.ppermute(array, axis, [(i, (i + shift) % n) for i in range(n)])


def ring4(array, axis):
    far = moved(array, axis, 2)
    one = moved(array, axis, 1)
    back = moved(array, axis, -1)
    return [array, one, far, back]


def norm_kernel(*refs):
    normed, rows = refs[4:6]
    held, sems = refs[6:10], refs[10]
    copies = [pltpu.make_async_copy(refs[i], held[i], sems.at[i]) for i in range(4)]
    for copy in copies:
        copy.start()
    for value, gain, out in ((0, 1, normed), (2, 3, rows)):
        copies[value].wait()
        copies[gain].wait()
        out[...] = norm_rows(held[value][...], held[gain][...]).astype(BF)


def normed_inputs(*arrays):
    target, _, source, _ = arrays
    return pl.pallas_call(
        norm_kernel,
        out_shape=[jax.ShapeDtypeStruct(a.shape, BF) for a in (target, source)],
        in_specs=[ANY] * 4,
        out_specs=[VMEM] * 2,
        scratch_shapes=[pltpu.VMEM(a.shape, a.dtype) for a in arrays]
        + [pltpu.SemaphoreType.DMA((4,))],
    )(*arrays)


def key_value_kernel(*refs):
    blocks = refs[:NX]
    own_w, other_w, kept_out, sent_out, rows, sems = refs[NX:]
    x = lax.axis_index("x")
    first = lax.axis_index("c") == 0
    copies = []
    for k in range(NX):
        place = pl.multiple_of(lax.rem(x - k + NX, NX) * 64, 64)
        copies.append(pltpu.make_async_copy(blocks[k], rows.at[pl.ds(place, 64), :], sems.at[k]))
    for copy in copies:
        copy.start()
    for copy in copies:
        copy.wait()

    def projected(weight):
        return lax.dot_general(
            weight[...], rows[...], (((1,), (1,)), ((), ())), preferred_element_type=F32)

    own, other = projected(own_w), projected(other_w)
    low = jnp.where(first, own, other)
    high = jnp.where(first, other, own)
    keys = jnp.concatenate([low[:64], high[:64]], axis=0).T
    turned = jnp.concatenate([low[64:], high[64:]], axis=0)
    values = jnp.concatenate([turned[:, :128], turned[:, 128:]], axis=0)
    kept_out[...] = jnp.where(first, keys, values).astype(BF)
    sent_out[...] = jnp.where(first, values, keys).astype(BF)


def key_value(blocks, own_w, other_w):
    return pl.pallas_call(
        key_value_kernel,
        out_shape=[jax.ShapeDtypeStruct((256, 128), BF)] * 2,
        in_specs=[ANY] * NX + [VMEM] * 2,
        out_specs=[VMEM] * 2,
        scratch_shapes=[pltpu.VMEM((256, 2048), BF), pltpu.SemaphoreType.DMA((NX,))],
        compiler_params=room(12),
        cost_estimate=pl.CostEstimate(
            flops=2 * 256 * 2048 * 256, bytes_accessed=3 << 20, transcendentals=0),
    )(*blocks, own_w, other_w)


def query_kernel(*refs):
    weight, out, held, rows, full, sems = refs[2 * NX :]
    x = lax.axis_index("x")
    copies = [pltpu.make_async_copy(weight, held, sems.at[0])]
    for i, block in enumerate(refs[: 2 * NX]):
        copies.append(pltpu.make_async_copy(block, rows.at[pl.ds(i * 16, 16), :], sems.at[i + 1]))
    for copy in copies:
        copy.start()
    for copy in copies:
        copy.wait()
    full[...] = jnp.dot(rows[...], held[...], preferred_element_type=F32)
    for k in range(NX):
        place = pl.multiple_of(lax.rem(x - k + NX, NX) * 128, 128)
        out[:, pl.ds(k * 128, 128)] = full[:, pl.ds(place, 128)].astype(BF)


def query_rows(blocks, weight):
    return pl.pallas_call(
        query_kernel,
        out_shape=jax.ShapeDtypeStruct((128, HD), BF),
        in_specs=[ANY] * (2 * NX + 1),
        out_specs=VMEM,
        scratch_shapes=[
            pltpu.VMEM((2048, HD), BF), pltpu.VMEM((128, 2048), BF), pltpu.VMEM((128, HD), F32),
            pltpu.SemaphoreType.DMA((2 * NX + 1,))],
        compiler_params=room(60),
        cost_estimate=pl.CostEstimate(
            flops=2 * 128 * 2048 * HD, bytes_accessed=3 << 20, transcendentals=0),
    )(*blocks, weight)


def soft_part(q, keys, values, outs, arrivals):
    scores = []
    for m in range(NY):
        if arrivals:
            arrivals[m].wait()
        block = jnp.concatenate([keys[m][k] for k in range(NX)], axis=1)
        scores.append(lax.dot_general(
            block, q, (((1,), (1,)), ((), ())), preferred_element_type=F32) * HD ** (-0.5))
    top = functools.reduce(
        jnp.maximum, [jnp.max(score, axis=0, keepdims=True) for score in scores])
    for arrival in arrivals[NY:]:
        arrival.wait()
    total, numerator = 0.0, 0.0
    for m in range(NY):
        weights = jnp.exp(scores[m] - top)
        total = total + jnp.sum(weights, axis=0, keepdims=True)
        block = jnp.concatenate([
            jnp.concatenate(
                [values[k][m, pl.ds(row, 128), :] for row in (256, 384, 0, 128)], axis=1)
            for k in range(NX)], axis=0)
        numerator = numerator + jnp.dot(
            block, weights.astype(BF), preferred_element_type=F32)
    part = numerator / total
    for side, out in enumerate(outs):
        cols = slice(side * 128, side * 128 + 128)
        out[pl.ds(0, HD), :] = part[:, cols].astype(BF)
        pieces = []
        for stat in (top[:, cols], total[:, cols]):
            for _ in range(3):
                piece = stat.astype(BF).astype(F32)
                pieces.append(piece)
                stat = stat - piece
        pieces.append(jnp.zeros((EXTRA - 6, 128), F32))
        out[pl.ds(HD, EXTRA), :] = jnp.concatenate(pieces, axis=0).astype(BF)


def attend_kernel(n, *refs):
    queries, refs = refs[:n], refs[n:]
    near, other = refs[:NX], refs[NX : 2 * NX]
    outs = refs[2 * NX : -3]
    keys, values, sems = refs[-3:]
    core = lax.axis_index("c")

    def copies(key_blocks, value_blocks):
        return [
            pltpu.make_async_copy(block, place.at[i], sems.at[side * 4 + i])
            for side, (blocks, place) in enumerate(((key_blocks, keys), (value_blocks, values)))
            for i, block in enumerate(blocks)]

    @pl.when(core == 0)
    def _():
        for copy in copies(near, other):
            copy.start()

    @pl.when(core == 1)
    def _():
        for copy in copies(other, near):
            copy.start()

    arrivals = copies(near, other)
    for i in range(0, n, 2):
        q = jnp.concatenate([query[...] for query in queries[i : i + 2]], axis=0)
        soft_part(q, keys, values, outs[i : i + 2], arrivals if i == 0 else [])


def attend(shifts, queries, near, other):
    n = len(shifts)
    return dict(zip(shifts, pl.pallas_call(
        functools.partial(attend_kernel, n),
        out_shape=[jax.ShapeDtypeStruct((HD + EXTRA, 128), BF)] * n,
        in_specs=[VMEM] * n + [ANY] * 8,
        out_specs=[VMEM] * n,
        scratch_shapes=[pltpu.VMEM((4, 4, 512, 128), BF)] * 2 + [pltpu.SemaphoreType.DMA((8,))],
        compiler_params=room(28),
        cost_estimate=pl.CostEstimate(
            flops=4 * 128 * n * 2048 * HD, bytes_accessed=4 << 20,
            transcendentals=n * 128 * 2048),
    )(*[queries[k] for k in shifts], *near, *other)))


def combine_kernel(*refs):
    arrived = refs[:NZ]
    weight, kept, sent, attended = refs[NZ:]
    x = lax.axis_index("x")
    tops, totals = [], []
    for part in arrived:
        stats = part[pl.ds(HD, EXTRA), :].astype(F32)
        tops.append(stats[0:1] + stats[1:2] + stats[2:3])
        totals.append(stats[3:4] + stats[4:5] + stats[5:6])
    top = functools.reduce(jnp.maximum, tops)
    shares = [total * jnp.exp(t - top) for t, total in zip(tops, totals)]
    whole = sum(shares)
    shares = [share / whole for share in shares]
    for k in range(NX):
        block = sum(
            part[pl.ds(k * 128, 128), :].astype(F32) * share
            for part, share in zip(arrived, shares))
        place = pl.multiple_of(lax.rem(x - k + NX, NX) * 128, 128)
        attended[:, pl.ds(place, 128)] = block.T.astype(BF)
    projected = jnp.dot(attended[...], weight[...], preferred_element_type=F32)
    for k in range(NX):
        kept[pl.ds(k * 16, 16), :] = projected[k * 32 : k * 32 + 16]
        sent[pl.ds(k * 16, 16), :] = projected[k * 32 + 16 : k * 32 + 32].astype(BF)


def combine(arrived, weight):
    return pl.pallas_call(
        combine_kernel,
        out_shape=[jax.ShapeDtypeStruct((64, 2048), F32), jax.ShapeDtypeStruct((64, 2048), BF)],
        in_specs=[VMEM] * (NZ + 1),
        out_specs=[VMEM] * 2,
        scratch_shapes=[pltpu.VMEM((128, HD), BF)],
        compiler_params=room(16),
        cost_estimate=pl.CostEstimate(
            flops=2 * 128 * 2048 * HD, bytes_accessed=4 << 20, transcendentals=1024),
    )(*arrived, weight)


def pair_kernel(kept, met, own, *outs):
    own[...] = kept[pl.ds(0, 16), :] + met[pl.ds(0, 16), :].astype(F32)
    for k, out in enumerate(outs, 1):
        rows = pl.ds(k * 16, 16)
        out[...] = (kept[rows, :] + met[rows, :].astype(F32)).astype(BF)


def pair_sum(kept, met):
    return pl.pallas_call(
        pair_kernel,
        out_shape=[jax.ShapeDtypeStruct((16, 2048), F32)]
        + [jax.ShapeDtypeStruct((16, 2048), BF)] * 3,
        in_specs=[VMEM] * 2,
        out_specs=[VMEM] * 4,
        compiler_params=room(8),
    )(kept, met)


def last_kernel(target, own, one, two, three, gain, out):
    stream = target[...].astype(F32) + (
        own[...] + one[...].astype(F32) + two[...].astype(F32) + three[...].astype(F32))
    out[...] = norm_rows(stream, gain[...]).astype(BF)


def last_norm(*arrays):
    return pl.pallas_call(
        last_kernel,
        out_shape=jax.ShapeDtypeStruct((16, 2048), BF),
        in_specs=[VMEM] * 6,
        out_specs=VMEM,
        compiler_params=room(8),
    )(*arrays)


def by_role(array, shift, axes):
    pairs = []
    for y in range(NY):
        for x in range(NX):
            for core, axis in enumerate(axes):
                to_y = (y + shift) % NY if axis == "y" else y
                to_x = (x + shift) % NX if axis == "x" else x
                pairs.append((((y * NX) + x) * NC + core, ((to_y * NX) + to_x) * NC + core))
    return lax.ppermute(array, ("y", "x", "c"), pairs)


def role_ring4(array, axes):
    far = by_role(array, 2, axes)
    one = by_role(array, 1, axes)
    back = by_role(array, -1, axes)
    return [array, one, far, back]


def on_device(target, source, target_gain, source_gain, w_query, w_key, w_value, w_out, final_gain):
    normed, rows = normed_inputs(target, target_gain, source, source_gain)
    own_targets = ring4(normed, "x")
    row_blocks = ring4(rows, "x")
    targets = [t for own in own_targets for t in (own, moved(own, "c", 1))]
    query = query_rows(targets, w_query[0])
    queries = {0: query}
    for shifts in ((4,), (3, 5), (2, 6, 1, 7)):
        for k in shifts:
            queries[k] = moved(query, "z", k)

    own_w = jnp.concatenate([w_key[0].T, w_value[0].T], axis=0)
    other_w = moved(own_w, "c", 1)

    piece, sent = key_value(row_blocks, own_w, other_w)
    piece = jnp.concatenate([piece, moved(sent, "c", 1)], axis=0)
    line = jnp.stack(role_ring4(piece, ("x", "y")))
    near = role_ring4(line, ("y", "x"))
    other = [moved(block, "c", 1) for block in near]


    parts, arrived = {}, []
    for shifts in ((3, 5), (4, 2, 6, 1), (7, 0)):
        parts.update(attend(shifts, queries, near, other))
        for k in shifts:
            if k:
                arrived.append(moved(parts[k], "z", -k))
    arrived.append(parts[0])
    kept, sent = combine(arrived, w_out[0])
    met = moved(sent, "c", 1)
    own, one, two, three = pair_sum(kept, met)
    two = moved(two, "x", -2)
    one = moved(one, "x", -1)
    three = moved(three, "x", -3)
    return last_norm(target, own, one, two, three, final_gain.reshape(1, -1))


def solution(mesh):
    grid = Mesh(mesh.devices.reshape(NZ, NY, NX, NC), ("z", "y", "x", "c"))
    every = P(("z", "y", "x", "c"), None)
    in_specs = (
        every, every, P(), P(),
        P(None, None, ("x", "c")), P(None, None, ("x", "c")), P(None, None, ("x", "c")),
        P(None, ("x", "c"), None), P(),
    )
    return jax.shard_map(
        on_device, mesh=grid, in_specs=in_specs, out_specs=every, check_vma=False)
```

```python
import functools

import jax
import jax.numpy as jnp
from jax import lax
from jax.experimental import pallas as pl
from jax.experimental.pallas import tpu as pltpu
from jax.sharding import Mesh, PartitionSpec as P

HD = 512
EPSILON = 1e-06
BF = jnp.bfloat16
F32 = jnp.float32
NZ, NY, NX, NC = 8, 4, 4, 2
EXTRA = 16
VMEM = pl.BlockSpec(memory_space=pltpu.VMEM)
ANY = pl.BlockSpec(memory_space=pl.ANY)


def room(mib):
    return pltpu.CompilerParams(vmem_limit_bytes=mib << 20)


def norm_rows(matrix, gain):
    values32 = matrix.astype(F32)
    scale = lax.rsqrt(jnp.mean(values32 * values32, axis=-1, keepdims=True) + EPSILON)
    return values32 * scale * gain


def moved(array, axis, shift):
    n = lax.axis_size(axis)
    return lax.ppermute(array, axis, [(i, (i + shift) % n) for i in range(n)])


def ring4(array, axis):
    far = moved(array, axis, 2)
    one = moved(array, axis, 1)
    back = moved(array, axis, -1)
    return [array, one, far, back]


def norm_kernel(*refs):
    normed, rows = refs[4:6]
    held, sems = refs[6:10], refs[10]
    copies = [pltpu.make_async_copy(refs[i], held[i], sems.at[i]) for i in range(4)]
    for copy in copies:
        copy.start()
    for value, gain, out in ((0, 1, normed), (2, 3, rows)):
        copies[value].wait()
        copies[gain].wait()
        out[...] = norm_rows(held[value][...], held[gain][...]).astype(BF)


def normed_inputs(*arrays):
    target, _, source, _ = arrays
    return pl.pallas_call(
        norm_kernel,
        out_shape=[jax.ShapeDtypeStruct(a.shape, BF) for a in (target, source)],
        in_specs=[ANY] * 4,
        out_specs=[VMEM] * 2,
        scratch_shapes=[pltpu.VMEM(a.shape, a.dtype) for a in arrays]
        + [pltpu.SemaphoreType.DMA((4,))],
    )(*arrays)


def key_value_kernel(*refs):
    blocks = refs[:NX]
    own_w, other_w, kept_out, sent_out, rows, sems = refs[NX:]
    x = lax.axis_index("x")
    first = lax.axis_index("c") == 0
    copies = []
    for k in range(NX):
        place = pl.multiple_of(lax.rem(x - k + NX, NX) * 64, 64)
        copies.append(pltpu.make_async_copy(blocks[k], rows.at[pl.ds(place, 64), :], sems.at[k]))
    for copy in copies:
        copy.start()
    for copy in copies:
        copy.wait()

    def projected(weight):
        return lax.dot_general(
            weight[...], rows[...], (((1,), (1,)), ((), ())), preferred_element_type=F32)

    own, other = projected(own_w), projected(other_w)
    low = jnp.where(first, own, other)
    high = jnp.where(first, other, own)
    keys = jnp.concatenate([low[:64], high[:64]], axis=0).T
    turned = jnp.concatenate([low[64:], high[64:]], axis=0)
    values = jnp.concatenate([turned[:, :128], turned[:, 128:]], axis=0)
    kept_out[...] = jnp.where(first, keys, values).astype(BF)
    sent_out[...] = jnp.where(first, values, keys).astype(BF)


def key_value(blocks, own_w, other_w):
    return pl.pallas_call(
        key_value_kernel,
        out_shape=[jax.ShapeDtypeStruct((256, 128), BF)] * 2,
        in_specs=[ANY] * NX + [VMEM] * 2,
        out_specs=[VMEM] * 2,
        scratch_shapes=[pltpu.VMEM((256, 2048), BF), pltpu.SemaphoreType.DMA((NX,))],
        compiler_params=room(12),
        cost_estimate=pl.CostEstimate(
            flops=2 * 256 * 2048 * 256, bytes_accessed=3 << 20, transcendentals=0),
    )(*blocks, own_w, other_w)


def query_kernel(*refs):
    weight, out, held, rows, full, sems = refs[2 * NX :]
    x = lax.axis_index("x")
    copies = [pltpu.make_async_copy(weight, held, sems.at[0])]
    for i, block in enumerate(refs[: 2 * NX]):
        copies.append(pltpu.make_async_copy(block, rows.at[pl.ds(i * 16, 16), :], sems.at[i + 1]))
    for copy in copies:
        copy.start()
    for copy in copies:
        copy.wait()
    full[...] = jnp.dot(rows[...], held[...], preferred_element_type=F32)
    for k in range(NX):
        place = pl.multiple_of(lax.rem(x - k + NX, NX) * 128, 128)
        out[:, pl.ds(k * 128, 128)] = full[:, pl.ds(place, 128)].astype(BF)


def query_rows(blocks, weight):
    return pl.pallas_call(
        query_kernel,
        out_shape=jax.ShapeDtypeStruct((128, HD), BF),
        in_specs=[ANY] * (2 * NX + 1),
        out_specs=VMEM,
        scratch_shapes=[
            pltpu.VMEM((2048, HD), BF), pltpu.VMEM((128, 2048), BF), pltpu.VMEM((128, HD), F32),
            pltpu.SemaphoreType.DMA((2 * NX + 1,))],
        compiler_params=room(60),
        cost_estimate=pl.CostEstimate(
            flops=2 * 128 * 2048 * HD, bytes_accessed=3 << 20, transcendentals=0),
    )(*blocks, weight)


def write_part(out, part, top, total):
    out[pl.ds(0, HD), :] = part.astype(BF)
    pieces = []
    for stat in (top, total):
        for _ in range(3):
            piece = stat.astype(BF).astype(F32)
            pieces.append(piece)
            stat = stat - piece
    pieces.append(jnp.zeros((EXTRA - 6, 128), F32))
    out[pl.ds(HD, EXTRA), :] = jnp.concatenate(pieces, axis=0).astype(BF)


def shares_of(parts):
    tops, totals = [], []
    for part in parts:
        stats = part[pl.ds(HD, EXTRA), :].astype(F32)
        tops.append(stats[0:1] + stats[1:2] + stats[2:3])
        totals.append(stats[3:4] + stats[4:5] + stats[5:6])
    top = functools.reduce(jnp.maximum, tops)
    shares = [total * jnp.exp(t - top) for t, total in zip(tops, totals)]
    whole = functools.reduce(jnp.add, shares)
    return [share / whole for share in shares], top, whole


def merge_kernel(*refs):
    n = len(refs) // 3
    for i in range(n):
        own, met, out = refs[i], refs[n + i], refs[2 * n + i]
        (first, second), top, total = shares_of((own, met))
        part = own[pl.ds(0, HD), :].astype(F32) * first + met[pl.ds(0, HD), :].astype(F32) * second
        write_part(out, part, top, total)


def merged(own, met):
    n = len(own)
    return pl.pallas_call(
        merge_kernel,
        out_shape=[jax.ShapeDtypeStruct((HD + EXTRA, 128), BF)] * n,
        in_specs=[VMEM] * (2 * n),
        out_specs=[VMEM] * n,
        compiler_params=room(8),
    )(*own, *met)


def soft_part(q, keys, values, outs, arrivals, scores, numerator):
    width = q.shape[0]
    for arrival in arrivals[:NY]:
        arrival.wait()

    def score_step(m, top):
        block = jnp.concatenate([keys[m, k] for k in range(NX)], axis=1)
        scores[m] = lax.dot_general(
            block, q, (((1,), (1,)), ((), ())), preferred_element_type=F32) * HD ** (-0.5)
        return jnp.maximum(top, jnp.max(scores[m], axis=0, keepdims=True))

    top = lax.fori_loop(0, NY, score_step, jnp.full((1, width), -jnp.inf, F32))
    for arrival in arrivals[NY:]:
        arrival.wait()
    numerator[...] = jnp.zeros_like(numerator)

    def weight_step(m, total):
        weights = jnp.exp(scores[m] - top)
        block = jnp.concatenate([
            jnp.concatenate(
                [values[k, m, pl.ds(row, 128), :] for row in (256, 384, 0, 128)], axis=1)
            for k in range(NX)], axis=0)
        numerator[...] += jnp.dot(block, weights.astype(BF), preferred_element_type=F32)
        return total + jnp.sum(weights, axis=0, keepdims=True)

    total = lax.fori_loop(0, NY, weight_step, jnp.zeros((1, width), F32))
    for side, out in enumerate(outs):
        cols = slice(side * 128, side * 128 + 128)
        write_part(out, numerator[:, cols] / total[:, cols], top[:, cols], total[:, cols])


def attend_kernel(n, *refs):
    queries, refs = refs[:n], refs[n:]
    near, other = refs[:NX], refs[NX : 2 * NX]
    outs = refs[2 * NX : 2 * NX + n]
    keys, values, sems = refs[2 * NX + n : 2 * NX + n + 3]
    work = refs[2 * NX + n + 3 :]
    core = lax.axis_index("c")

    def copies(key_blocks, value_blocks):
        return [
            pltpu.make_async_copy(block, place.at[i], sems.at[side * 4 + i])
            for side, (blocks, place) in enumerate(((key_blocks, keys), (value_blocks, values)))
            for i, block in enumerate(blocks)]

    @pl.when(core == 0)
    def _():
        for copy in copies(near, other):
            copy.start()

    @pl.when(core == 1)
    def _():
        for copy in copies(other, near):
            copy.start()

    arrivals = copies(near, other)
    for i in range(0, n, 2):
        q = jnp.concatenate([query[...] for query in queries[i : i + 2]], axis=0)
        soft_part(q, keys, values, outs[i : i + 2], arrivals if i == 0 else [], *work)


def attend(shifts, queries, near, other):
    n = len(shifts)
    work = [pltpu.VMEM((4, 512, 256), F32), pltpu.VMEM((HD, 256), F32)]
    return dict(zip(shifts, pl.pallas_call(
        functools.partial(attend_kernel, n),
        out_shape=[jax.ShapeDtypeStruct((HD + EXTRA, 128), BF)] * n,
        in_specs=[VMEM] * n + [ANY] * 8,
        out_specs=[VMEM] * n,
        scratch_shapes=[pltpu.VMEM((4, 4, 512, 128), BF)] * 2 + [
            pltpu.SemaphoreType.DMA((8,))] + work,
        compiler_params=room(28),
        cost_estimate=pl.CostEstimate(
            flops=4 * 128 * n * 2048 * HD, bytes_accessed=4 << 20,
            transcendentals=n * 128 * 2048),
    )(*[queries[k] for k in shifts], *near, *other)))


def combine_kernel(*refs):
    arrived = refs[:3]
    weight, kept, sent, attended = refs[3:]
    x = lax.axis_index("x")
    shares, _, _ = shares_of(arrived)
    for k in range(NX):
        block = sum(
            part[pl.ds(k * 128, 128), :].astype(F32) * share
            for part, share in zip(arrived, shares))
        place = pl.multiple_of(lax.rem(x - k + NX, NX) * 128, 128)
        attended[:, pl.ds(place, 128)] = block.T.astype(BF)
    projected = jnp.dot(attended[...], weight[...], preferred_element_type=F32)
    for k in range(NX):
        kept[pl.ds(k * 16, 16), :] = projected[k * 32 : k * 32 + 16]
        sent[pl.ds(k * 16, 16), :] = projected[k * 32 + 16 : k * 32 + 32].astype(BF)


def combine(arrived, weight):
    return pl.pallas_call(
        combine_kernel,
        out_shape=[jax.ShapeDtypeStruct((64, 2048), F32), jax.ShapeDtypeStruct((64, 2048), BF)],
        in_specs=[VMEM] * 4,
        out_specs=[VMEM] * 2,
        scratch_shapes=[pltpu.VMEM((128, HD), BF)],
        compiler_params=room(16),
        cost_estimate=pl.CostEstimate(
            flops=2 * 128 * 2048 * HD, bytes_accessed=4 << 20, transcendentals=1024),
    )(*arrived, weight)


def pair_kernel(kept, met, own, *outs):
    own[...] = kept[pl.ds(0, 16), :] + met[pl.ds(0, 16), :].astype(F32)
    for k, out in enumerate(outs, 1):
        rows = pl.ds(k * 16, 16)
        out[...] = (kept[rows, :] + met[rows, :].astype(F32)).astype(BF)


def pair_sum(kept, met):
    return pl.pallas_call(
        pair_kernel,
        out_shape=[jax.ShapeDtypeStruct((16, 2048), F32)]
        + [jax.ShapeDtypeStruct((16, 2048), BF)] * 3,
        in_specs=[VMEM] * 2,
        out_specs=[VMEM] * 4,
        compiler_params=room(8),
    )(kept, met)


def last_kernel(target, own, one, two, three, gain, out):
    stream = target[...].astype(F32) + (
        own[...] + one[...].astype(F32) + two[...].astype(F32) + three[...].astype(F32))
    out[...] = norm_rows(stream, gain[...]).astype(BF)


def last_norm(*arrays):
    return pl.pallas_call(
        last_kernel,
        out_shape=jax.ShapeDtypeStruct((16, 2048), BF),
        in_specs=[VMEM] * 6,
        out_specs=VMEM,
        compiler_params=room(8),
    )(*arrays)


def by_role(array, shift, axes):
    pairs = []
    for y in range(NY):
        for x in range(NX):
            for core, axis in enumerate(axes):
                to_y = (y + shift) % NY if axis == "y" else y
                to_x = (x + shift) % NX if axis == "x" else x
                pairs.append((((y * NX) + x) * NC + core, ((to_y * NX) + to_x) * NC + core))
    return lax.ppermute(array, ("y", "x", "c"), pairs)


def role_ring4(array, axes):
    far = by_role(array, 2, axes)
    one = by_role(array, 1, axes)
    back = by_role(array, -1, axes)
    return [array, one, far, back]


def on_device(target, source, target_gain, source_gain, w_query, w_key, w_value, w_out, final_gain):
    normed, rows = normed_inputs(target, target_gain, source, source_gain)
    own_targets = ring4(normed, "x")
    row_blocks = ring4(rows, "x")
    targets = [t for own in own_targets for t in (own, moved(own, "c", 1))]
    query = query_rows(targets, w_query[0])
    queries = {0: query}
    for shifts in ((4,), (3, 5), (2, 6, 1, 7)):
        for k in shifts:
            queries[k] = moved(query, "z", k)

    own_w = jnp.concatenate([w_key[0].T, w_value[0].T], axis=0)
    other_w = moved(own_w, "c", 1)

    piece, sent = key_value(row_blocks, own_w, other_w)
    piece = jnp.concatenate([piece, moved(sent, "c", 1)], axis=0)
    line = jnp.stack(role_ring4(piece, ("x", "y")))
    near = role_ring4(line, ("y", "x"))
    other = [moved(block, "c", 1) for block in near]


    sums = []
    for step, shifts in enumerate(((4, 3), (5, 2), (6, 1), (7, 0))):
        parts = attend(shifts, queries, near, other)
        if step == 0:
            sums = [parts[4], parts[3]]
        elif step < 3:
            sums = list(merged([parts[k] for k in shifts], sums))
        else:
            sums[0] = merged([parts[7]], sums[:1])[0]
        sums[0] = moved(sums[0], "z", 1)
        if step < 3:
            sums[1] = moved(sums[1], "z", -1)
    last = parts[0]
    kept, sent = combine([last] + sums, w_out[0])
    met = moved(sent, "c", 1)
    own, one, two, three = pair_sum(kept, met)
    two = moved(two, "x", -2)
    one = moved(one, "x", -1)
    three = moved(three, "x", -3)
    return last_norm(target, own, one, two, three, final_gain.reshape(1, -1))


def solution(mesh):
    grid = Mesh(mesh.devices.reshape(NZ, NY, NX, NC), ("z", "y", "x", "c"))
    every = P(("z", "y", "x", "c"), None)
    in_specs = (
        every, every, P(), P(),
        P(None, None, ("x", "c")), P(None, None, ("x", "c")), P(None, None, ("x", "c")),
        P(None, ("x", "c"), None), P(),
    )
    return jax.shard_map(
        on_device, mesh=grid, in_specs=in_specs, out_specs=every, check_vma=False)
```

```python
import functools

import jax
import jax.numpy as jnp
from jax import lax
from jax.experimental import pallas as pl
from jax.experimental.pallas import tpu as pltpu
from jax.sharding import Mesh, PartitionSpec as P

HD = 512
EPSILON = 1e-06
BF = jnp.bfloat16
F32 = jnp.float32
NZ, NY, NX, NC = 8, 4, 4, 2
EXTRA = 16
ROOM_A, ROOM_B = 16, 12
VMEM = pl.BlockSpec(memory_space=pltpu.VMEM)
ANY = pl.BlockSpec(memory_space=pl.ANY)


def room(mib):
    return pltpu.CompilerParams(vmem_limit_bytes=mib << 20)


def norm_rows(matrix, gain):
    values32 = matrix.astype(F32)
    scale = lax.rsqrt(jnp.mean(values32 * values32, axis=-1, keepdims=True) + EPSILON)
    return values32 * scale * gain


def moved(array, axis, shift):
    n = lax.axis_size(axis)
    return lax.ppermute(array, axis, [(i, (i + shift) % n) for i in range(n)])


def ring4(array, axis):
    far = moved(array, axis, 2)
    one = moved(array, axis, 1)
    back = moved(array, axis, -1)
    return [array, one, far, back]


def norm_kernel(*refs):
    normed, rows = refs[4:6]
    held, sems = refs[6:10], refs[10]
    copies = [pltpu.make_async_copy(refs[i], held[i], sems.at[i]) for i in range(4)]
    for copy in copies:
        copy.start()
    for value, gain, out in ((0, 1, normed), (2, 3, rows)):
        copies[value].wait()
        copies[gain].wait()
        out[...] = norm_rows(held[value][...], held[gain][...]).astype(BF)


def normed_inputs(*arrays):
    target, _, source, _ = arrays
    return pl.pallas_call(
        norm_kernel,
        out_shape=[jax.ShapeDtypeStruct(a.shape, BF) for a in (target, source)],
        in_specs=[ANY] * 4,
        out_specs=[VMEM] * 2,
        scratch_shapes=[pltpu.VMEM(a.shape, a.dtype) for a in arrays]
        + [pltpu.SemaphoreType.DMA((4,))],
    )(*arrays)


def key_value_kernel(*refs):
    blocks = refs[:NX]
    own_w, other_w, kept_out, sent_out, rows, sems = refs[NX:]
    x = lax.axis_index("x")
    first = lax.axis_index("c") == 0
    copies = []
    for k in range(NX):
        place = pl.multiple_of(lax.rem(x - k + NX, NX) * 64, 64)
        copies.append(pltpu.make_async_copy(blocks[k], rows.at[pl.ds(place, 64), :], sems.at[k]))
    for copy in copies:
        copy.start()
    for copy in copies:
        copy.wait()

    def projected(weight):
        return lax.dot_general(
            weight[...], rows[...], (((1,), (1,)), ((), ())), preferred_element_type=F32)

    own, other = projected(own_w), projected(other_w)
    low = jnp.where(first, own, other)
    high = jnp.where(first, other, own)
    keys = jnp.concatenate([low[:64], high[:64]], axis=0).T
    turned = jnp.concatenate([low[64:], high[64:]], axis=0)
    values = jnp.concatenate([turned[:, :128], turned[:, 128:]], axis=0)
    kept_out[...] = jnp.where(first, keys, values).astype(BF)
    sent_out[...] = jnp.where(first, values, keys).astype(BF)


def key_value(blocks, own_w, other_w):
    return pl.pallas_call(
        key_value_kernel,
        out_shape=[jax.ShapeDtypeStruct((256, 128), BF)] * 2,
        in_specs=[ANY] * NX + [VMEM] * 2,
        out_specs=[VMEM] * 2,
        scratch_shapes=[pltpu.VMEM((256, 2048), BF), pltpu.SemaphoreType.DMA((NX,))],
        compiler_params=room(12),
        cost_estimate=pl.CostEstimate(
            flops=2 * 256 * 2048 * 256, bytes_accessed=3 << 20, transcendentals=0),
    )(*blocks, own_w, other_w)


def query_kernel(*refs):
    weight, out, held, rows, full, sems = refs[2 * NX :]
    x = lax.axis_index("x")
    copies = [pltpu.make_async_copy(weight, held, sems.at[0])]
    for i, block in enumerate(refs[: 2 * NX]):
        copies.append(pltpu.make_async_copy(block, rows.at[pl.ds(i * 16, 16), :], sems.at[i + 1]))
    for copy in copies:
        copy.start()
    for copy in copies:
        copy.wait()
    full[...] = jnp.dot(rows[...], held[...], preferred_element_type=F32)
    for k in range(NX):
        place = pl.multiple_of(lax.rem(x - k + NX, NX) * 128, 128)
        out[:, pl.ds(k * 128, 128)] = full[:, pl.ds(place, 128)].astype(BF)


def query_rows(blocks, weight):
    return pl.pallas_call(
        query_kernel,
        out_shape=jax.ShapeDtypeStruct((128, HD), BF),
        in_specs=[ANY] * (2 * NX + 1),
        out_specs=VMEM,
        scratch_shapes=[
            pltpu.VMEM((2048, HD), BF), pltpu.VMEM((128, 2048), BF), pltpu.VMEM((128, HD), F32),
            pltpu.SemaphoreType.DMA((2 * NX + 1,))],
        compiler_params=room(60),
        cost_estimate=pl.CostEstimate(
            flops=2 * 128 * 2048 * HD, bytes_accessed=3 << 20, transcendentals=0),
    )(*blocks, weight)


def write_part(out, part, top, total):
    out[pl.ds(0, HD), :] = part.astype(BF)
    pieces = []
    for stat in (top, total):
        for _ in range(3):
            piece = stat.astype(BF).astype(F32)
            pieces.append(piece)
            stat = stat - piece
    pieces.append(jnp.zeros((EXTRA - 6, 128), F32))
    out[pl.ds(HD, EXTRA), :] = jnp.concatenate(pieces, axis=0).astype(BF)


def shares_of(parts):
    tops, totals = [], []
    for part in parts:
        stats = part[pl.ds(HD, EXTRA), :].astype(F32)
        tops.append(stats[0:1] + stats[1:2] + stats[2:3])
        totals.append(stats[3:4] + stats[4:5] + stats[5:6])
    top = functools.reduce(jnp.maximum, tops)
    shares = [total * jnp.exp(t - top) for t, total in zip(tops, totals)]
    whole = functools.reduce(jnp.add, shares)
    return [share / whole for share in shares], top, whole


def merge_kernel(*refs):
    n = len(refs) // 3
    for i in range(n):
        own, met, out = refs[i], refs[n + i], refs[2 * n + i]
        (first, second), top, total = shares_of((own, met))
        part = own[pl.ds(0, HD), :].astype(F32) * first + met[pl.ds(0, HD), :].astype(F32) * second
        write_part(out, part, top, total)


def merged(own, met):
    n = len(own)
    return pl.pallas_call(
        merge_kernel,
        out_shape=[jax.ShapeDtypeStruct((HD + EXTRA, 128), BF)] * n,
        in_specs=[VMEM] * (2 * n),
        out_specs=[VMEM] * n,
        compiler_params=room(8),
    )(*own, *met)


def soft_part(q, keys, values, outs, arrivals, scores, numerator):
    width = q.shape[0]
    for arrival in arrivals[:NY]:
        arrival.wait()

    def score_step(m, top):
        block = jnp.concatenate([keys[m, k] for k in range(NX)], axis=1)
        scores[m] = lax.dot_general(
            block, q, (((1,), (1,)), ((), ())), preferred_element_type=F32) * HD ** (-0.5)
        return jnp.maximum(top, jnp.max(scores[m], axis=0, keepdims=True))

    top = lax.fori_loop(0, NY, score_step, jnp.full((1, width), -jnp.inf, F32))
    for arrival in arrivals[NY:]:
        arrival.wait()
    numerator[...] = jnp.zeros_like(numerator)

    def weight_step(m, total):
        weights = jnp.exp(scores[m] - top)
        block = jnp.concatenate([
            jnp.concatenate(
                [values[k, m, pl.ds(row, 128), :] for row in (256, 384, 0, 128)], axis=1)
            for k in range(NX)], axis=0)
        numerator[...] += jnp.dot(block, weights.astype(BF), preferred_element_type=F32)
        return total + jnp.sum(weights, axis=0, keepdims=True)

    total = lax.fori_loop(0, NY, weight_step, jnp.zeros((1, width), F32))
    for side, out in enumerate(outs):
        cols = slice(side * 128, side * 128 + 128)
        write_part(out, numerator[:, cols] / total[:, cols], top[:, cols], total[:, cols])


def first_kernel(query, *refs):
    near, other = refs[:NX], refs[NX : 2 * NX]
    out, keys, values, sems, scores, numerator = refs[2 * NX :]
    core = lax.axis_index("c")

    def copies(key_blocks, value_blocks):
        return [
            pltpu.make_async_copy(block, place.at[i], sems.at[side * 4 + i])
            for side, (blocks, place) in enumerate(((key_blocks, keys), (value_blocks, values)))
            for i, block in enumerate(blocks)]

    @pl.when(core == 0)
    def _():
        for copy in copies(near, other):
            copy.start()

    @pl.when(core == 1)
    def _():
        for copy in copies(other, near):
            copy.start()

    soft_part(query[...], keys, values, [out], copies(near, other), scores, numerator)


def work_for(n):
    return [pltpu.VMEM((4, 512, 128 * n), F32), pltpu.VMEM((HD, 128 * n), F32)]


def cost_of(n):
    return pl.CostEstimate(
        flops=4 * 128 * n * 2048 * HD, bytes_accessed=4 << 20, transcendentals=n * 128 * 2048)


def attend_first(query, near, other):
    held = jax.ShapeDtypeStruct((4, 4, 512, 128), BF)
    return pl.pallas_call(
        first_kernel,
        out_shape=[jax.ShapeDtypeStruct((HD + EXTRA, 128), BF), held, held],
        in_specs=[VMEM] + [ANY] * 8,
        out_specs=[VMEM] * 3,
        scratch_shapes=[pltpu.SemaphoreType.DMA((8,))] + work_for(1),
        compiler_params=room(ROOM_A),
        cost_estimate=cost_of(1),
    )(query, *near, *other)


def attend_kernel(n, *refs):
    keys, values = refs[n : n + 2]
    outs, work = refs[n + 2 : 2 * n + 2], refs[2 * n + 2 :]
    q = jnp.concatenate([query[...] for query in refs[:n]], axis=0)
    soft_part(q, keys, values, outs, [], *work)


def attend(queries, keys, values):
    n = len(queries)
    return pl.pallas_call(
        functools.partial(attend_kernel, n),
        out_shape=[jax.ShapeDtypeStruct((HD + EXTRA, 128), BF)] * n,
        in_specs=[VMEM] * (n + 2),
        out_specs=[VMEM] * n,
        scratch_shapes=work_for(n),
        compiler_params=room(ROOM_B),
        cost_estimate=cost_of(n),
    )(*queries, keys, values)


def combine_kernel(*refs):
    arrived = refs[:3]
    weight, kept, sent, attended = refs[3:]
    x = lax.axis_index("x")
    shares, _, _ = shares_of(arrived)
    for k in range(NX):
        block = sum(
            part[pl.ds(k * 128, 128), :].astype(F32) * share
            for part, share in zip(arrived, shares))
        place = pl.multiple_of(lax.rem(x - k + NX, NX) * 128, 128)
        attended[:, pl.ds(place, 128)] = block.T.astype(BF)
    projected = jnp.dot(attended[...], weight[...], preferred_element_type=F32)
    for k in range(NX):
        kept[pl.ds(k * 16, 16), :] = projected[k * 32 : k * 32 + 16]
        sent[pl.ds(k * 16, 16), :] = projected[k * 32 + 16 : k * 32 + 32].astype(BF)


def combine(arrived, weight):
    return pl.pallas_call(
        combine_kernel,
        out_shape=[jax.ShapeDtypeStruct((64, 2048), F32), jax.ShapeDtypeStruct((64, 2048), BF)],
        in_specs=[VMEM] * 4,
        out_specs=[VMEM] * 2,
        scratch_shapes=[pltpu.VMEM((128, HD), BF)],
        compiler_params=room(16),
        cost_estimate=pl.CostEstimate(
            flops=2 * 128 * 2048 * HD, bytes_accessed=4 << 20, transcendentals=1024),
    )(*arrived, weight)


def pair_kernel(kept, met, own, *outs):
    own[...] = kept[pl.ds(0, 16), :] + met[pl.ds(0, 16), :].astype(F32)
    for k, out in enumerate(outs, 1):
        rows = pl.ds(k * 16, 16)
        out[...] = (kept[rows, :] + met[rows, :].astype(F32)).astype(BF)


def pair_sum(kept, met):
    return pl.pallas_call(
        pair_kernel,
        out_shape=[jax.ShapeDtypeStruct((16, 2048), F32)]
        + [jax.ShapeDtypeStruct((16, 2048), BF)] * 3,
        in_specs=[VMEM] * 2,
        out_specs=[VMEM] * 4,
        compiler_params=room(8),
    )(kept, met)


def last_kernel(target, own, one, two, three, gain, out):
    stream = target[...].astype(F32) + (
        own[...] + one[...].astype(F32) + two[...].astype(F32) + three[...].astype(F32))
    out[...] = norm_rows(stream, gain[...]).astype(BF)


def last_norm(*arrays):
    return pl.pallas_call(
        last_kernel,
        out_shape=jax.ShapeDtypeStruct((16, 2048), BF),
        in_specs=[VMEM] * 6,
        out_specs=VMEM,
        compiler_params=room(8),
    )(*arrays)


def by_role(array, shift, axes):
    pairs = []
    for y in range(NY):
        for x in range(NX):
            for core, axis in enumerate(axes):
                to_y = (y + shift) % NY if axis == "y" else y
                to_x = (x + shift) % NX if axis == "x" else x
                pairs.append((((y * NX) + x) * NC + core, ((to_y * NX) + to_x) * NC + core))
    return lax.ppermute(array, ("y", "x", "c"), pairs)


def role_ring4(array, axes):
    far = by_role(array, 2, axes)
    one = by_role(array, 1, axes)
    back = by_role(array, -1, axes)
    return [array, one, far, back]


def on_device(target, source, target_gain, source_gain, w_query, w_key, w_value, w_out, final_gain):
    normed, rows = normed_inputs(target, target_gain, source, source_gain)
    own_targets = ring4(normed, "x")
    row_blocks = ring4(rows, "x")
    targets = [t for own in own_targets for t in (own, moved(own, "c", 1))]
    query = query_rows(targets, w_query[0])
    queries = {0: query}
    for shifts in ((4,), (3, 5), (2, 6, 1, 7)):
        for k in shifts:
            queries[k] = moved(query, "z", k)

    own_w = jnp.concatenate([w_key[0].T, w_value[0].T], axis=0)
    other_w = moved(own_w, "c", 1)

    piece, sent = key_value(row_blocks, own_w, other_w)
    piece = jnp.concatenate([piece, moved(sent, "c", 1)], axis=0)
    line = jnp.stack(role_ring4(piece, ("x", "y")))
    near = role_ring4(line, ("y", "x"))
    other = [moved(block, "c", 1) for block in near]


    for step, shifts in enumerate(((4,), (5, 3), (6, 2), (7, 1), (0,))):
        blocks = [queries[k] for k in shifts]
        if step == 0:
            ahead, keys, values = attend_first(*blocks, near, other)
        else:
            parts = attend(blocks, keys, values)
        if step in (1, 2, 3):
            ahead = merged(parts[:1], [ahead])[0]
        if step == 1:
            behind = parts[1]
        elif step in (2, 3):
            behind = merged(parts[1:], [behind])[0]
        if step < 4:
            ahead = moved(ahead, "z", 1)
        if step in (1, 2, 3):
            behind = moved(behind, "z", -1)
    kept, sent = combine([parts[0], ahead, behind], w_out[0])
    met = moved(sent, "c", 1)
    own, one, two, three = pair_sum(kept, met)
    two = moved(two, "x", -2)
    one = moved(one, "x", -1)
    three = moved(three, "x", -3)
    return last_norm(target, own, one, two, three, final_gain.reshape(1, -1))


def solution(mesh):
    grid = Mesh(mesh.devices.reshape(NZ, NY, NX, NC), ("z", "y", "x", "c"))
    every = P(("z", "y", "x", "c"), None)
    in_specs = (
        every, every, P(), P(),
        P(None, None, ("x", "c")), P(None, None, ("x", "c")), P(None, None, ("x", "c")),
        P(None, ("x", "c"), None), P(),
    )
    return jax.shard_map(
        on_device, mesh=grid, in_specs=in_specs, out_specs=every, check_vma=False)
```

```python
import functools

import jax
import jax.numpy as jnp
from jax import lax
from jax.experimental import pallas as pl
from jax.experimental.pallas import tpu as pltpu
from jax.sharding import Mesh, PartitionSpec as P

HD = 512
EPSILON = 1e-06
BF = jnp.bfloat16
F32 = jnp.float32
NZ, NY, NX, NC = 8, 4, 4, 2
EXTRA = 16
ROOM_A, ROOM_B = 16, 12
VMEM = pl.BlockSpec(memory_space=pltpu.VMEM)
ANY = pl.BlockSpec(memory_space=pl.ANY)


def room(mib):
    return pltpu.CompilerParams(vmem_limit_bytes=mib << 20)


def norm_rows(matrix, gain):
    values32 = matrix.astype(F32)
    scale = lax.rsqrt(jnp.mean(values32 * values32, axis=-1, keepdims=True) + EPSILON)
    return values32 * scale * gain


def moved(array, axis, shift):
    n = lax.axis_size(axis)
    return lax.ppermute(array, axis, [(i, (i + shift) % n) for i in range(n)])


def ring4(array, axis):
    far = moved(array, axis, 2)
    one = moved(array, axis, 1)
    back = moved(array, axis, -1)
    return [array, one, far, back]


def norm_kernel(*refs):
    normed, rows = refs[4:6]
    held, sems = refs[6:10], refs[10]
    copies = [pltpu.make_async_copy(refs[i], held[i], sems.at[i]) for i in range(4)]
    for copy in copies:
        copy.start()
    for value, gain, out in ((0, 1, normed), (2, 3, rows)):
        copies[value].wait()
        copies[gain].wait()
        out[...] = norm_rows(held[value][...], held[gain][...]).astype(BF)


def normed_inputs(*arrays):
    target, _, source, _ = arrays
    return pl.pallas_call(
        norm_kernel,
        out_shape=[jax.ShapeDtypeStruct(a.shape, BF) for a in (target, source)],
        in_specs=[ANY] * 4,
        out_specs=[VMEM] * 2,
        scratch_shapes=[pltpu.VMEM(a.shape, a.dtype) for a in arrays]
        + [pltpu.SemaphoreType.DMA((4,))],
    )(*arrays)


def key_value_kernel(*refs):
    blocks = refs[:NX]
    own_w, other_w, kept_out, sent_out, rows, sems = refs[NX:]
    x = lax.axis_index("x")
    first = lax.axis_index("c") == 0
    copies = []
    for k in range(NX):
        place = pl.multiple_of(lax.rem(x - k + NX, NX) * 64, 64)
        copies.append(pltpu.make_async_copy(blocks[k], rows.at[pl.ds(place, 64), :], sems.at[k]))
    for copy in copies:
        copy.start()
    for copy in copies:
        copy.wait()

    def projected(weight):
        return lax.dot_general(
            weight[...], rows[...], (((1,), (1,)), ((), ())), preferred_element_type=F32)

    own, other = projected(own_w), projected(other_w)
    low = jnp.where(first, own, other)
    high = jnp.where(first, other, own)
    keys = jnp.concatenate([low[:64], high[:64]], axis=0).T
    turned = jnp.concatenate([low[64:], high[64:]], axis=0)
    values = jnp.concatenate([turned[:, :128], turned[:, 128:]], axis=0)
    kept_out[...] = jnp.where(first, keys, values).astype(BF)
    sent_out[...] = jnp.where(first, values, keys).astype(BF)


def key_value(blocks, own_w, other_w):
    return pl.pallas_call(
        key_value_kernel,
        out_shape=[jax.ShapeDtypeStruct((256, 128), BF)] * 2,
        in_specs=[ANY] * NX + [VMEM] * 2,
        out_specs=[VMEM] * 2,
        scratch_shapes=[pltpu.VMEM((256, 2048), BF), pltpu.SemaphoreType.DMA((NX,))],
        compiler_params=room(12),
        cost_estimate=pl.CostEstimate(
            flops=2 * 256 * 2048 * 256, bytes_accessed=3 << 20, transcendentals=0),
    )(*blocks, own_w, other_w)


def query_kernel(*refs):
    weight, out, held, rows, full, sems = refs[2 * NX :]
    x = lax.axis_index("x")
    copies = [pltpu.make_async_copy(weight, held, sems.at[0])]
    for i, block in enumerate(refs[: 2 * NX]):
        copies.append(pltpu.make_async_copy(block, rows.at[pl.ds(i * 16, 16), :], sems.at[i + 1]))
    for copy in copies:
        copy.start()
    for copy in copies:
        copy.wait()
    full[...] = jnp.dot(rows[...], held[...], preferred_element_type=F32)
    for k in range(NX):
        place = pl.multiple_of(lax.rem(x - k + NX, NX) * 128, 128)
        out[:, pl.ds(k * 128, 128)] = full[:, pl.ds(place, 128)].astype(BF)


def query_rows(blocks, weight):
    return pl.pallas_call(
        query_kernel,
        out_shape=jax.ShapeDtypeStruct((128, HD), BF),
        in_specs=[ANY] * (2 * NX + 1),
        out_specs=VMEM,
        scratch_shapes=[
            pltpu.VMEM((2048, HD), BF), pltpu.VMEM((128, 2048), BF), pltpu.VMEM((128, HD), F32),
            pltpu.SemaphoreType.DMA((2 * NX + 1,))],
        compiler_params=room(60),
        cost_estimate=pl.CostEstimate(
            flops=2 * 128 * 2048 * HD, bytes_accessed=3 << 20, transcendentals=0),
    )(*blocks, weight)


def write_part(out, part, top, total):
    out[pl.ds(0, HD), :] = part.astype(BF)
    pieces = []
    for stat in (top, total):
        for _ in range(3):
            piece = stat.astype(BF).astype(F32)
            pieces.append(piece)
            stat = stat - piece
    pieces.append(jnp.zeros((EXTRA - 6, 128), F32))
    out[pl.ds(HD, EXTRA), :] = jnp.concatenate(pieces, axis=0).astype(BF)


def shares_of(parts):
    tops, totals = [], []
    for part in parts:
        stats = part[pl.ds(HD, EXTRA), :].astype(F32)
        tops.append(stats[0:1] + stats[1:2] + stats[2:3])
        totals.append(stats[3:4] + stats[4:5] + stats[5:6])
    top = functools.reduce(jnp.maximum, tops)
    shares = [total * jnp.exp(t - top) for t, total in zip(tops, totals)]
    whole = functools.reduce(jnp.add, shares)
    return [share / whole for share in shares], top, whole


def merge_kernel(*refs):
    n = len(refs) // 3
    for i in range(n):
        own, met, out = refs[i], refs[n + i], refs[2 * n + i]
        (first, second), top, total = shares_of((own, met))
        part = own[pl.ds(0, HD), :].astype(F32) * first + met[pl.ds(0, HD), :].astype(F32) * second
        write_part(out, part, top, total)


def merged(own, met):
    n = len(own)
    return pl.pallas_call(
        merge_kernel,
        out_shape=[jax.ShapeDtypeStruct((HD + EXTRA, 128), BF)] * n,
        in_specs=[VMEM] * (2 * n),
        out_specs=[VMEM] * n,
        compiler_params=room(8),
    )(*own, *met)


def soft_part(q, keys, values, outs, arrivals, scores, numerator, rounded):
    width = q.shape[0]
    for arrival in arrivals[:NY]:
        arrival.wait()

    def score_step(m, top):
        block = jnp.concatenate([keys[m, k] for k in range(NX)], axis=1)
        scores[m] = lax.dot_general(
            block, q, (((1,), (1,)), ((), ())), preferred_element_type=F32) * HD ** (-0.5)
        return jnp.maximum(top, jnp.max(scores[m], axis=0, keepdims=True))

    top = lax.fori_loop(0, NY, score_step, jnp.full((1, width), -jnp.inf, F32))
    for arrival in arrivals[NY:]:
        arrival.wait()

    def weight_step(m, total):
        weights = jnp.exp(scores[m] - top)
        rounded[m] = weights.astype(BF)
        return total + jnp.sum(weights, axis=0, keepdims=True)

    total = lax.fori_loop(0, NY, weight_step, jnp.zeros((1, width), F32))

    def value_step(pair, carry):
        block = jnp.concatenate([
            jnp.concatenate([
                values[2 * pair + k, m, pl.ds(row, 128), :]
                for m in range(NY) for row in (256, 384, 0, 128)], axis=1)
            for k in range(2)], axis=0)
        numerator[pl.ds(pl.multiple_of(pair * 256, 256), 256), :] = jnp.dot(
            block, rounded[...].reshape(2048, width), preferred_element_type=F32)
        return carry

    lax.fori_loop(0, 2, value_step, 0)
    for side, out in enumerate(outs):
        cols = slice(side * 128, side * 128 + 128)
        write_part(out, numerator[:, cols] / total[:, cols], top[:, cols], total[:, cols])


def first_kernel(query, *refs):
    near, other = refs[:NX], refs[NX : 2 * NX]
    out, keys, values, sems, *work = refs[2 * NX :]
    core = lax.axis_index("c")

    def copies(key_blocks, value_blocks):
        return [
            pltpu.make_async_copy(block, place.at[i], sems.at[side * 4 + i])
            for side, (blocks, place) in enumerate(((key_blocks, keys), (value_blocks, values)))
            for i, block in enumerate(blocks)]

    @pl.when(core == 0)
    def _():
        for copy in copies(near, other):
            copy.start()

    @pl.when(core == 1)
    def _():
        for copy in copies(other, near):
            copy.start()

    soft_part(query[...], keys, values, [out], copies(near, other), *work)


def work_for(n):
    return [
        pltpu.VMEM((4, 512, 128 * n), F32), pltpu.VMEM((HD, 128 * n), F32),
        pltpu.VMEM((4, 512, 128 * n), BF)]


def cost_of(n):
    return pl.CostEstimate(
        flops=4 * 128 * n * 2048 * HD, bytes_accessed=4 << 20, transcendentals=n * 128 * 2048)


def attend_first(query, near, other):
    held = jax.ShapeDtypeStruct((4, 4, 512, 128), BF)
    return pl.pallas_call(
        first_kernel,
        out_shape=[jax.ShapeDtypeStruct((HD + EXTRA, 128), BF), held, held],
        in_specs=[VMEM] + [ANY] * 8,
        out_specs=[VMEM] * 3,
        scratch_shapes=[pltpu.SemaphoreType.DMA((8,))] + work_for(1),
        compiler_params=room(ROOM_A),
        cost_estimate=cost_of(1),
    )(query, *near, *other)


def attend_kernel(n, *refs):
    keys, values = refs[n : n + 2]
    outs, work = refs[n + 2 : 2 * n + 2], refs[2 * n + 2 :]
    q = jnp.concatenate([query[...] for query in refs[:n]], axis=0)
    soft_part(q, keys, values, outs, [], *work)


def attend(queries, keys, values):
    n = len(queries)
    return pl.pallas_call(
        functools.partial(attend_kernel, n),
        out_shape=[jax.ShapeDtypeStruct((HD + EXTRA, 128), BF)] * n,
        in_specs=[VMEM] * (n + 2),
        out_specs=[VMEM] * n,
        scratch_shapes=work_for(n),
        compiler_params=room(ROOM_B),
        cost_estimate=cost_of(n),
    )(*queries, keys, values)


def combine_kernel(*refs):
    arrived = refs[:3]
    weight, kept, sent, attended = refs[3:]
    x = lax.axis_index("x")
    shares, _, _ = shares_of(arrived)
    for k in range(NX):
        block = sum(
            part[pl.ds(k * 128, 128), :].astype(F32) * share
            for part, share in zip(arrived, shares))
        place = pl.multiple_of(lax.rem(x - k + NX, NX) * 128, 128)
        attended[:, pl.ds(place, 128)] = block.T.astype(BF)
    projected = jnp.dot(attended[...], weight[...], preferred_element_type=F32)
    for k in range(NX):
        kept[pl.ds(k * 16, 16), :] = projected[k * 32 : k * 32 + 16]
        sent[pl.ds(k * 16, 16), :] = projected[k * 32 + 16 : k * 32 + 32].astype(BF)


def combine(arrived, weight):
    return pl.pallas_call(
        combine_kernel,
        out_shape=[jax.ShapeDtypeStruct((64, 2048), F32), jax.ShapeDtypeStruct((64, 2048), BF)],
        in_specs=[VMEM] * 4,
        out_specs=[VMEM] * 2,
        scratch_shapes=[pltpu.VMEM((128, HD), BF)],
        compiler_params=room(16),
        cost_estimate=pl.CostEstimate(
            flops=2 * 128 * 2048 * HD, bytes_accessed=4 << 20, transcendentals=1024),
    )(*arrived, weight)


def pair_kernel(kept, met, own, *outs):
    own[...] = kept[pl.ds(0, 16), :] + met[pl.ds(0, 16), :].astype(F32)
    for k, out in enumerate(outs, 1):
        rows = pl.ds(k * 16, 16)
        out[...] = (kept[rows, :] + met[rows, :].astype(F32)).astype(BF)


def pair_sum(kept, met):
    return pl.pallas_call(
        pair_kernel,
        out_shape=[jax.ShapeDtypeStruct((16, 2048), F32)]
        + [jax.ShapeDtypeStruct((16, 2048), BF)] * 3,
        in_specs=[VMEM] * 2,
        out_specs=[VMEM] * 4,
        compiler_params=room(8),
    )(kept, met)


def last_kernel(target, own, one, two, three, gain, out):
    stream = target[...].astype(F32) + (
        own[...] + one[...].astype(F32) + two[...].astype(F32) + three[...].astype(F32))
    out[...] = norm_rows(stream, gain[...]).astype(BF)


def last_norm(*arrays):
    return pl.pallas_call(
        last_kernel,
        out_shape=jax.ShapeDtypeStruct((16, 2048), BF),
        in_specs=[VMEM] * 6,
        out_specs=VMEM,
        compiler_params=room(8),
    )(*arrays)


def by_role(array, shift, axes):
    pairs = []
    for y in range(NY):
        for x in range(NX):
            for core, axis in enumerate(axes):
                to_y = (y + shift) % NY if axis == "y" else y
                to_x = (x + shift) % NX if axis == "x" else x
                pairs.append((((y * NX) + x) * NC + core, ((to_y * NX) + to_x) * NC + core))
    return lax.ppermute(array, ("y", "x", "c"), pairs)


def role_ring4(array, axes):
    far = by_role(array, 2, axes)
    one = by_role(array, 1, axes)
    back = by_role(array, -1, axes)
    return [array, one, far, back]


def on_device(target, source, target_gain, source_gain, w_query, w_key, w_value, w_out, final_gain):
    normed, rows = normed_inputs(target, target_gain, source, source_gain)
    own_targets = ring4(normed, "x")
    row_blocks = ring4(rows, "x")
    targets = [t for own in own_targets for t in (own, moved(own, "c", 1))]
    query = query_rows(targets, w_query[0])
    queries = {0: query}
    for shifts in ((4,), (3, 5), (2, 6, 1, 7)):
        for k in shifts:
            queries[k] = moved(query, "z", k)

    own_w = jnp.concatenate([w_key[0].T, w_value[0].T], axis=0)
    other_w = moved(own_w, "c", 1)

    piece, sent = key_value(row_blocks, own_w, other_w)
    piece = jnp.concatenate([piece, moved(sent, "c", 1)], axis=0)
    line = jnp.stack(role_ring4(piece, ("x", "y")))
    near = role_ring4(line, ("y", "x"))
    other = [moved(block, "c", 1) for block in near]


    for step, shifts in enumerate(((4,), (5, 3), (6, 2), (7, 1), (0,))):
        blocks = [queries[k] for k in shifts]
        if step == 0:
            ahead, keys, values = attend_first(*blocks, near, other)
        else:
            parts = attend(blocks, keys, values)
        if step in (1, 2, 3):
            ahead = merged(parts[:1], [ahead])[0]
        if step == 1:
            behind = parts[1]
        elif step in (2, 3):
            behind = merged(parts[1:], [behind])[0]
        if step < 4:
            ahead = moved(ahead, "z", 1)
        if step in (1, 2, 3):
            behind = moved(behind, "z", -1)
    kept, sent = combine([parts[0], ahead, behind], w_out[0])
    met = moved(sent, "c", 1)
    own, one, two, three = pair_sum(kept, met)
    two = moved(two, "x", -2)
    one = moved(one, "x", -1)
    three = moved(three, "x", -3)
    return last_norm(target, own, one, two, three, final_gain.reshape(1, -1))


def solution(mesh):
    grid = Mesh(mesh.devices.reshape(NZ, NY, NX, NC), ("z", "y", "x", "c"))
    every = P(("z", "y", "x", "c"), None)
    in_specs = (
        every, every, P(), P(),
        P(None, None, ("x", "c")), P(None, None, ("x", "c")), P(None, None, ("x", "c")),
        P(None, ("x", "c"), None), P(),
    )
    return jax.shard_map(
        on_device, mesh=grid, in_specs=in_specs, out_specs=every, check_vma=False)
```
